32 devices in a mesh: kv: 16 (over z, y, x), tp: 2 (over core).
Axes of the slice: x: 2, y: 2, z: 4, core: 2. Of those that a mesh axis runs over, the one named last changes fastest.
Arguments:
- tokens: bfloat16 [128, 2048], P(None, ('kv', 'tp')), may hold values from -16 to 16
- mix_gain: float32 [2048], P('kv'), may hold values from 0.1 to 1.9
- query_weight: bfloat16 [2048, 2048], P('kv', 'tp'), may hold values from -0.125 to 0.125
- key_weight: bfloat16 [2048, 2048], P('kv', 'tp'), may hold values from -0.125 to 0.125
- value_weight: bfloat16 [2048, 2048], P('kv', 'tp'), may hold values from -0.125 to 0.125
- beta_weight: bfloat16 [2048, 16], P('kv', 'tp'), may hold values from -0.125 to 0.125
- decay_weight: bfloat16 [2048, 16], P('kv', 'tp'), may hold values from -0.125 to 0.125
- decay_rate: float32 [16], P('tp'), may hold values from 0.05 to 1
- prior_state: float32 [128, 16, 128, 128], P('kv', 'tp'), may hold values from -1.5 to 1.5
- tail_keys: bfloat16 [128, 16, 64, 128], P('kv', 'tp'), may hold values from -6 to 6
- tail_values: bfloat16 [128, 16, 64, 128], P('kv', 'tp'), may hold values from -6 to 6
- tail_beta: float32 [128, 16, 64], P('kv', 'tp'), may hold values from 0.1 to 0.9
- tail_decay: float32 [128, 16, 64], P('kv', 'tp'), may hold values from -2 to 0
- lengths: int32 [128], P('kv'), may hold values from 1 to 64, 3276 in all
- out_weight: bfloat16 [2048, 2048], P('tp', 'kv'), may hold values from -0.375 to 0.375
- mlp_gain: float32 [2048], P('kv'), may hold values from 0.1 to 1.9
- up_weight: bfloat16 [2048, 8192], P('kv', 'tp'), may hold values from -0.125 to 0.125
- down_weight: bfloat16 [8192, 2048], P('tp', 'kv'), may hold values from -0.0625 to 0.0625
Outputs:
- mixed: bfloat16 [128, 2048], P(None, ('kv', 'tp'))
The draws below stay inside these ranges and needn't reach their ends.
All inputs are finite; a program needn't handle non-finite values. No bound on the sum of `lengths` on one device may be relied on, other than what follows from the above.
Results may differ from the reference program's by a relative error of at most 0.013.
Values may be sent and summed in bfloat16 or wider, within the bound.
A program may use at most 64 MiB of HBM per device.

```python
import math
import jax
import jax.numpy as jnp
import numpy as np
from jax import lax

D = 2048
HEAD_COUNT = 16
HEAD_DIM = 128
FF = 8192
PENDING_KEYS = 64
INNER = 2048
SEQUENCE_BATCH = 128


def draw_tokens(key, part):
    first = jax.random.fold_in(key, 11)
    second = jax.random.fold_in(key, 12)
    base = jax.random.normal(first, (SEQUENCE_BATCH, D), jnp.float32)
    column = jnp.arange(D, dtype=jnp.float32) / D
    rising = jnp.exp(math.log(6.0) * (column - 0.5)) * jax.random.uniform(second, (D,), jnp.float32, 0.6, 1.4)
    value_vectors = base * rising[None, :]
    return jnp.clip(value_vectors, -16.0, 16.0).astype(jnp.bfloat16)


def draw_tail_decay(key, part):
    pick_key = jax.random.fold_in(key, 21)
    slow_key = jax.random.fold_in(key, 22)
    quick_key = jax.random.fold_in(key, 23)
    factor_key = jax.random.fold_in(key, 24)
    rough_key = jax.random.fold_in(key, 25)
    spike_random_key = jax.random.fold_in(key, 26)
    drop_key = jax.random.fold_in(key, 27)
    quick = jax.random.randint(pick_key, (HEAD_COUNT,), 0, 2) == 1
    slow_rate = jnp.exp(jax.random.uniform(slow_key, (HEAD_COUNT,), jnp.float32, math.log(0.001), math.log(0.005)))
    quick_rate = jnp.exp(jax.random.uniform(quick_key, (HEAD_COUNT,), jnp.float32, math.log(0.04), math.log(0.1)))
    per_head_rate = jnp.where(quick, quick_rate, slow_rate)
    sequence_multiplier = jnp.exp(jax.random.uniform(factor_key, (SEQUENCE_BATCH, 1, 1), jnp.float32, math.log(0.5), math.log(2.0)))
    jitter_amount = jax.random.uniform(rough_key, (SEQUENCE_BATCH, HEAD_COUNT, PENDING_KEYS), jnp.float32, 0.5, 1.5)
    spike_sample = jax.random.randint(spike_random_key, (SEQUENCE_BATCH, HEAD_COUNT, PENDING_KEYS), 0, 32) == 0
    discard_fraction = jnp.log(jax.random.uniform(drop_key, (SEQUENCE_BATCH, HEAD_COUNT, PENDING_KEYS), jnp.float32, 0.5, 0.8))
    value_vectors = -per_head_rate[None, :, None] * sequence_multiplier * jitter_amount + jnp.where(spike_sample, discard_fraction, 0.0)
    return jnp.clip(value_vectors, -2.0, 0.0)


def levels(rng, extent, pieces, smallest, top_value):
    loudness = 1.0
    for axis_at, parts in pieces:
        draws = jax.random.uniform(jax.random.fold_in(jax.random.fold_in(rng, 6), axis_at), (parts,), jnp.float32, smallest / len(pieces), top_value / len(pieces))
        loudness = loudness * jnp.repeat(jnp.exp(draws), extent[axis_at] // parts).reshape((-1,) + (1,) * (len(extent) - 1 - axis_at))
    return loudness


def length_profile(count, total, reach, slope):
    weights = [(1 << 20) // math.isqrt(grade ** slope) + 1 for grade in range(2, count + 1)]
    rest, given = total - reach - (count - 1), [1] * (count - 1)
    while rest > 0:
        movable = [i for i in range(count - 1) if given[i] < reach]
        pool, remaining = sum([weights[i] for i in movable]), rest
        for i in movable:
            more = min(reach - given[i], max(1, remaining * weights[i] // pool), rest)
            given[i] = given[i] + more
            rest = rest - more
    return np.array([reach] + given)


def ragged(stream_key, count, total, reach, skew):
    if count == 2:
        one = jax.random.randint(stream_key, (), max(1, total - reach), min(reach, total - 1) + 1)
        return jnp.stack([one, total - one])
    sizes = jnp.asarray(length_profile(count, total, reach, skew), jnp.int32)
    couples = (count - 1) // 2
    source_of, receiver = sizes[1:1 + 2 * couples:2], sizes[2:2 + 2 * couples:2]
    room = jnp.minimum(source_of - 1, reach - receiver)
    passed = jax.random.randint(jax.random.fold_in(stream_key, 1), (couples,), 0, 1 << 20) % (room + 1)
    sizes = sizes.at[1:1 + 2 * couples:2].set(source_of - passed).at[2:2 + 2 * couples:2].set(receiver + passed)
    return sizes[jax.random.permutation(jax.random.fold_in(stream_key, 2), count)]


def gaussian(rng, dims, deviation, limit, cuts=(), held_as=jnp.bfloat16):
    drawn = deviation * jax.random.normal(rng, dims, jnp.float32)
    if cuts:
        drawn = drawn * levels(rng, dims, cuts, -0.22, 0.18)
    return jnp.clip(drawn, -limit, limit).astype(held_as)


def setup_inputs(seed: int = 0) -> dict:
    key_list = jax.random.split(jax.random.key(seed), 19)
    tokens = draw_tokens(jax.random.fold_in(key_list[18], 71), 0)
    mix_gain = jnp.clip(1.0 + 0.18 * jax.random.normal(key_list[1], (D,), jnp.float32), 0.1, 1.9)
    query_weight = gaussian(key_list[2], (D, INNER), D ** -0.5, 0.125, ((0, 16), (1, 2)))
    key_weight = gaussian(key_list[3], (D, INNER), D ** -0.5, 0.125, ((0, 16), (1, 2)))
    value_weight = gaussian(key_list[4], (D, INNER), D ** -0.5, 0.125, ((0, 16), (1, 2)))
    beta_weight = gaussian(key_list[5], (D, HEAD_COUNT), D ** -0.5, 0.125, ((0, 16), (1, 2)))
    decay_weight = gaussian(key_list[6], (D, HEAD_COUNT), D ** -0.5, 0.125, ((0, 16), (1, 2)))
    decay_rate = jnp.clip(jnp.exp(math.log(1.0) - 2.9957323 * jax.random.uniform(key_list[7], (HEAD_COUNT,), jnp.float32) ** levels(key_list[7], (HEAD_COUNT,), ((0, 2),), -0.2, 0.2)), 0.05, 1.0)
    prior_state = gaussian(key_list[8], (SEQUENCE_BATCH, HEAD_COUNT, HEAD_DIM, HEAD_DIM), 0.25, 1.5, ((0, 16), (1, 2)), jnp.float32)
    tail_keys = gaussian(key_list[9], (SEQUENCE_BATCH, HEAD_COUNT, PENDING_KEYS, HEAD_DIM), 1.0, 6.0, ((0, 16), (1, 2)))
    tail_values = gaussian(key_list[10], (SEQUENCE_BATCH, HEAD_COUNT, PENDING_KEYS, HEAD_DIM), 1.0, 6.0, ((0, 16), (1, 2)))
    tail_beta = jnp.clip(0.1 + 0.79999997 * jax.random.uniform(key_list[11], (SEQUENCE_BATCH, HEAD_COUNT, PENDING_KEYS), jnp.float32) ** levels(key_list[11], (SEQUENCE_BATCH, HEAD_COUNT, PENDING_KEYS), ((0, 16), (1, 2)), -0.2, 0.2), 0.1, 0.9)
    tail_decay = draw_tail_decay(jax.random.fold_in(key_list[18], 71), 0)
    lengths = ragged(key_list[13], SEQUENCE_BATCH, SEQUENCE_BATCH * PENDING_KEYS * 2 // 5, PENDING_KEYS, 2).astype(jnp.int32)
    out_weight = gaussian(key_list[14], (INNER, D), (INNER // 8) ** -0.5, 0.375, ((0, 2), (1, 16)))
    mlp_gain = jnp.clip(1.0 + 0.18 * jax.random.normal(key_list[15], (D,), jnp.float32), 0.1, 1.9)
    up_weight = gaussian(key_list[16], (D, FF), D ** -0.5, 0.125, ((0, 16), (1, 2)))
    down_weight = gaussian(key_list[17], (FF, D), FF ** -0.5, 0.0625, ((0, 2), (1, 16)))
    return dict(tokens=tokens, mix_gain=mix_gain, query_weight=query_weight, key_weight=key_weight, value_weight=value_weight, beta_weight=beta_weight, decay_weight=decay_weight, decay_rate=decay_rate, prior_state=prior_state, tail_keys=tail_keys, tail_values=tail_values, tail_beta=tail_beta, tail_decay=tail_decay, lengths=lengths, out_weight=out_weight, mlp_gain=mlp_gain, up_weight=up_weight, down_weight=down_weight)


epsilon = 1e-06

def unit_rows(vectors):
    return vectors * lax.rsqrt(lax.optimization_barrier(jnp.sum(vectors * vectors, axis=-1, keepdims=True)) + epsilon)

def delta_read(previous_state, keys, value_vectors, betas, decays, live_count, queries, new_key, new_value, new_beta, new_decay):
    peak_value = lax.Precision.HIGHEST
    positions = keys.shape[1]
    head_dim = keys.shape[2]
    live_mask = jnp.arange(positions, dtype=jnp.int32)[None, :] < live_count[:, None]
    unit_keys = unit_rows(keys.astype(jnp.float32))
    value_rows = value_vectors.astype(jnp.float32)
    beta_live = jnp.where(live_mask, betas, 0.0)
    decay_live = jnp.where(live_mask, decays, 0.0)
    cumulative = jnp.cumsum(decay_live, axis=1)
    row_index = jnp.arange(positions, dtype=jnp.int32)
    strict = (row_index[:, None] > row_index[None, :])[None]
    log_gap = cumulative[:, :, None] - cumulative[:, None, :]
    key_intersection = jnp.einsum('nik,njk->nij', unit_keys, unit_keys, precision=peak_value)
    lower_part = jnp.where(strict, beta_live[:, :, None] * jnp.exp(jnp.where(strict, log_gap, 0.0)) * key_intersection, 0.0)
    system = lower_part + jnp.eye(positions, dtype=jnp.float32)[None]
    right_sides = jnp.concatenate([(beta_live * jnp.exp(cumulative))[:, :, None] * unit_keys, beta_live[:, :, None] * value_rows], axis=2)
    solved = jax.scipy.linalg.solve_triangular(system, right_sides, lower=True, unit_diagonal=True)
    weight_matrix_rows = solved[:, :, :head_dim]
    unscaled_rows = solved[:, :, head_dim:]
    adjusted_result = unscaled_rows - jnp.einsum('mfd,mdx->mfx', weight_matrix_rows, previous_state, precision=peak_value)
    intersection = lax.optimization_barrier(jnp.sum(new_key * queries, axis=1))
    test_vector = queries - (new_beta * intersection)[:, None] * new_key
    total_decay = cumulative[:, -1]
    state_readout = jnp.einsum('rq,rqt->rt', test_vector, previous_state, precision=peak_value)
    tail_weights = jnp.exp(total_decay[:, None] - cumulative) * jnp.einsum('njk,nk->nj', unit_keys, test_vector, precision=peak_value)
    from_tail = jnp.einsum('nj,njv->nv', tail_weights, adjusted_result, precision=peak_value)
    readout = jnp.exp(total_decay)[:, None] * state_readout + from_tail
    return jnp.exp(new_decay)[:, None] * readout + (new_beta * intersection)[:, None] * new_value

def reference(tokens, mix_gain, query_weight, key_weight, value_weight, beta_weight, decay_weight, decay_rate, prior_state, tail_keys, tail_values, tail_beta, tail_decay, lengths, out_weight, mlp_gain, up_weight, down_weight):
    token_float = tokens.astype(jnp.float32)
    row_squares = lax.optimization_barrier(jnp.sum(token_float * token_float, axis=1, keepdims=True))
    row_scale = lax.rsqrt(row_squares / D + epsilon)
    normed = (token_float * mix_gain[None, :]).astype(jnp.bfloat16)

    def project(weight):
        return jnp.dot(normed.astype(jnp.float32), weight.astype(jnp.float32), preferred_element_type=jnp.float32) * row_scale

    def by_heads(raw):
        return raw.reshape(SEQUENCE_BATCH, HEAD_COUNT, HEAD_DIM)
    queries = unit_rows(jax.nn.silu(by_heads(project(query_weight))))
    new_keys = unit_rows(jax.nn.silu(by_heads(project(key_weight))))
    new_values = jax.nn.silu(by_heads(project(value_weight)))
    new_beta = jax.nn.sigmoid(project(beta_weight))
    new_decay = -decay_rate[None, :] * jax.nn.softplus(project(decay_weight))

    def one_head(operands):
        return delta_read(*operands)
    operands = (jnp.moveaxis(prior_state, 1, 0), jnp.moveaxis(tail_keys, 1, 0), jnp.moveaxis(tail_values, 1, 0), jnp.moveaxis(tail_beta, 1, 0), jnp.moveaxis(tail_decay, 1, 0), jnp.broadcast_to(lengths[None, :], (HEAD_COUNT, SEQUENCE_BATCH)), jnp.moveaxis(queries, 1, 0), jnp.moveaxis(new_keys, 1, 0), jnp.moveaxis(new_values, 1, 0), jnp.moveaxis(new_beta, 1, 0), jnp.moveaxis(new_decay, 1, 0))
    readout = jnp.moveaxis(lax.map(one_head, operands), 0, 1)
    head_out = readout.reshape(SEQUENCE_BATCH, INNER).astype(jnp.bfloat16)
    attended = jnp.dot(head_out.astype(jnp.float32), out_weight.astype(jnp.float32), preferred_element_type=jnp.float32)
    mixed_in = (token_float + attended).astype(jnp.bfloat16)
    mixed_float = mixed_in.astype(jnp.float32)
    mixer_squares = lax.optimization_barrier(jnp.sum(mixed_float * mixed_float, axis=1, keepdims=True))
    mixer_normed = (mixed_float * mlp_gain[None, :]).astype(jnp.bfloat16)
    hidden_raw = jnp.dot(mixer_normed.astype(jnp.float32), up_weight.astype(jnp.float32), preferred_element_type=jnp.float32) * lax.rsqrt(mixer_squares / D + epsilon)
    hidden = jnp.square(jnp.maximum(hidden_raw, 0.0)).astype(jnp.bfloat16)
    down = jnp.dot(hidden.astype(jnp.float32), down_weight.astype(jnp.float32), preferred_element_type=jnp.float32)
    return (mixed_float + down).astype(jnp.bfloat16)
```

```python
import functools

import jax
import jax.numpy as jnp
from jax import lax
from jax.experimental import pallas as pl
from jax.experimental.pallas import tpu as pltpu
from jax.sharding import PartitionSpec as P

epsilon = 1e-06
LINK = jnp.bfloat16
F32 = jnp.float32
MESH = pl.DeviceIdType.MESH


def peer_of(axis, offset, count):
    return lax.rem(lax.axis_index(axis) + offset, count)


def greet(groups):
    barrier = pltpu.get_barrier_semaphore()
    for axis, count in groups:
        for offset in range(1, count):
            pl.semaphore_signal(
                barrier, inc=1, device_id={axis: peer_of(axis, offset, count)}, device_id_type=MESH
            )


def greeted(groups):
    barrier = pltpu.get_barrier_semaphore()
    pl.semaphore_wait(barrier, sum(count - 1 for _, count in groups))


def send(src, dst, send_sem, recv_sem, axis, peer):
    copy = pltpu.make_async_remote_copy(
        src_ref=src,
        dst_ref=dst,
        send_sem=send_sem,
        recv_sem=recv_sem,
        device_id={axis: peer},
        device_id_type=MESH,
    )
    copy.start()
    return copy


def exchange_rows(parts, arrivals, send_sems, recv_sems, count):
    copies = []
    for offset in range(1, count):
        peer = peer_of("kv", offset, count)
        copies.append(
            send(parts.at[peer], arrivals.at[offset], send_sems.at[offset], recv_sems.at[offset], "kv", peer)
        )
    return copies


def gathered_sum(parts, arrivals, copies, count):
    total = parts[lax.axis_index("kv")].astype(F32)
    for offset in range(1, count):
        copies[offset - 1].wait_recv()
        total = total + arrivals[offset].astype(F32)
    return total


def split_rows(block, count):
    return block.reshape(count, block.shape[0] // count, block.shape[1])


def project_kernel(
    count,
    heads,
    tokens,
    gain,
    query_w,
    key_w,
    value_w,
    small_w,
    query_o,
    key_o,
    value_o,
    small_o,
    small_parts,
    small_in,
    parts,
    arrivals,
    send_sems,
    recv_sems,
):
    groups = (("kv", count),)
    greet(groups)
    token_float = tokens[...].astype(F32)
    normed = (token_float * gain[...]).astype(jnp.bfloat16)
    small = jnp.dot(normed, small_w[...], preferred_element_type=F32)
    squares = jnp.sum(token_float * token_float, axis=1, keepdims=True)
    lane = lax.broadcasted_iota(jnp.int32, small.shape, 1)
    small_parts[...] = split_rows(jnp.where(lane == 2 * heads, squares, small), count)
    greeted(groups)
    flights = [exchange_rows(small_parts, small_in, send_sems.at[3], recv_sems.at[3], count)]
    for index, weight in enumerate((query_w, key_w, value_w)):
        block = jnp.dot(normed, weight[...], preferred_element_type=F32)
        parts[index] = split_rows(block, count).astype(LINK)
        flights.append(
            exchange_rows(parts.at[index], arrivals.at[index], send_sems.at[index], recv_sems.at[index], count)
        )
    small_o[...] = gathered_sum(small_parts, small_in, flights[0], count)
    for index, out in enumerate((query_o, key_o, value_o)):
        out[...] = gathered_sum(parts.at[index], arrivals.at[index], flights[index + 1], count)
    for flight in flights:
        for copy in flight:
            copy.wait_send()


def unit_rows(vectors):
    return vectors * lax.rsqrt(jnp.sum(vectors * vectors, axis=-1, keepdims=True) + epsilon)


def silu(x):
    return x * jax.nn.sigmoid(x)


def softplus(x):
    return jnp.maximum(x, 0.0) + jnp.log(1.0 + jnp.exp(-jnp.abs(x)))


def delta_kernel(
    width,
    query_r,
    key_r,
    value_r,
    small_r,
    rate,
    lengths,
    betas,
    decays,
    keys,
    values,
    state,
    out,
    keys32,
    values32,
    rows_scr,
):
    rows, heads, head_dim = state.shape[0], state.shape[1], state.shape[2]
    span = betas.shape[2]

    def stack(pieces):
        return jnp.concatenate(pieces, axis=0)

    keys32[...] = keys[...].astype(F32)
    values32[...] = values[...].astype(F32)
    small = small_r[...]
    scale = lax.rsqrt(small[:, 2 * heads : 2 * heads + 1] / width + epsilon)
    scaled = small * scale

    def by_heads(ref):
        raw = ref[...] * scale
        return stack([raw[:, h * head_dim : (h + 1) * head_dim] for h in range(heads)])

    queries = unit_rows(silu(by_heads(query_r)))
    new_key = unit_rows(silu(by_heads(key_r)))
    new_value = silu(by_heads(value_r))
    new_beta = stack([jax.nn.sigmoid(scaled[:, h : h + 1]) for h in range(heads)])
    new_decay = stack(
        [-rate[0, h] * softplus(scaled[:, heads + h : heads + h + 1]) for h in range(heads)]
    )
    live = lax.broadcasted_iota(jnp.int32, (rows, span), 1) < lengths[...]
    beta_live = stack([jnp.where(live, betas[:, h, :], 0.0) for h in range(heads)])
    shrink = stack([jnp.exp(jnp.where(live, decays[:, h, :], 0.0)) for h in range(heads)])

    meet = new_beta * jnp.sum(new_key * queries, axis=1, keepdims=True)
    fade = jnp.exp(new_decay)
    probe = (queries - meet * new_key) * fade
    read = meet * new_value
    for t in range(span - 1, -1, -1):
        k = stack([keys32[pl.ds(h * span + t, rows, stride=heads * span), :] for h in range(heads)])
        v = stack([values32[pl.ds(h * span + t, rows, stride=heads * span), :] for h in range(heads)])
        inverse = lax.rsqrt(jnp.sum(k * k, axis=1, keepdims=True) + epsilon)
        unit = k * inverse
        hit = beta_live[:, t : t + 1] * jnp.sum(unit * probe, axis=1, keepdims=True)
        read = read + hit * v
        probe = shrink[:, t : t + 1] * (probe - hit * unit)
    total = rows * heads
    if total < head_dim:
        probe = jnp.concatenate([probe, jnp.zeros((head_dim - total, head_dim), F32)], axis=0)
    columns = probe.T
    for h in range(heads):
        for r in range(rows):
            n = h * rows + r
            rows_scr[n : n + 1, :] = jnp.sum(columns[:, n : n + 1] * state[r, h], axis=0, keepdims=True)
    final = read + rows_scr[...]
    for h in range(heads):
        out[:, h * head_dim : (h + 1) * head_dim] = final[h * rows : (h + 1) * rows].astype(jnp.bfloat16)


def across_heads(block, mine, arrivals, send_sems, recv_sems, count):
    mine[...] = block
    copies = []
    for offset in range(1, count):
        peer = peer_of("tp", offset, count)
        copies.append(send(mine, arrivals.at[offset], send_sems.at[offset], recv_sems.at[offset], "tp", peer))
    total = block
    for offset in range(1, count):
        copies[offset - 1].wait_recv()
        total = total + arrivals[offset]
    return total, copies


def spread(own, everywhere, send_sems, recv_sems, count):
    me = lax.axis_index("kv")
    return [
        send(own, everywhere.at[me], send_sems.at[offset], recv_sems.at[offset], "kv", peer_of("kv", offset, count))
        for offset in range(1, count)
    ]


def whole_rows(everywhere, dtype):
    block = everywhere[...].astype(F32)
    return block.reshape(block.shape[0] * block.shape[1], block.shape[2]).astype(dtype)


def mixer_kernel(
    count,
    tp_count,
    width,
    head_out,
    tokens,
    gain,
    out_w,
    up_w,
    down_w,
    result,
    heads_all,
    share,
    share_in,
    down_share,
    down_in,
    square_parts,
    square_in,
    parts,
    arrivals,
    hidden_own,
    hidden_all,
    kv_send,
    kv_recv,
    tp_send,
    tp_recv,
):
    groups = (("kv", count), ("tp", tp_count))
    pieces, piece = parts.shape[0], parts.shape[3]
    me = lax.axis_index("kv")
    greet(groups)
    heads_all[me] = head_out[...]
    greeted(groups)
    flights = [spread(head_out, heads_all, kv_send.at[0], kv_recv.at[0], count)]
    for copy in flights[0]:
        copy.wait_recv()
    attended = jnp.dot(whole_rows(heads_all, jnp.bfloat16), out_w[...], preferred_element_type=F32)
    attended, copies = across_heads(attended, share, share_in, tp_send.at[0], tp_recv.at[0], tp_count)
    flights.append(copies)
    mixed_in = (tokens[...].astype(F32) + attended).astype(jnp.bfloat16).astype(F32)
    squares = jnp.sum(mixed_in * mixed_in, axis=1, keepdims=True)
    square_parts[...] = split_rows(jnp.broadcast_to(squares, (squares.shape[0], 128)), count)
    square_flight = exchange_rows(square_parts, square_in, kv_send.at[1], kv_recv.at[1], count)
    normed = (mixed_in * gain[...]).astype(jnp.bfloat16)
    up_flights = []
    for p in range(pieces):
        block = jnp.dot(normed, up_w[:, p * piece : (p + 1) * piece], preferred_element_type=F32)
        parts[p] = split_rows(block, count).astype(LINK)
        up_flights.append(
            exchange_rows(parts.at[p], arrivals.at[p], kv_send.at[2 + p], kv_recv.at[2 + p], count)
        )
    own_squares = gathered_sum(square_parts, square_in, square_flight, count)
    scale = lax.rsqrt(own_squares[:, :1] / width + epsilon)
    down_flights = []
    for p in range(pieces):
        raw = gathered_sum(parts.at[p], arrivals.at[p], up_flights[p], count) * scale
        hidden = jnp.square(jnp.maximum(raw, 0.0)).astype(jnp.bfloat16)
        hidden_own[p] = hidden
        slot = 2 + pieces + p
        down_flights.append(
            spread(hidden_own.at[p], hidden_all.at[p], kv_send.at[slot], kv_recv.at[slot], count)
        )
        hidden_all[p, me] = hidden
    down = jnp.zeros(share.shape, F32)
    for p in range(pieces):
        for copy in down_flights[p]:
            copy.wait_recv()
        down = down + jnp.dot(
            whole_rows(hidden_all.at[p], jnp.bfloat16),
            down_w[p * piece : (p + 1) * piece, :],
            preferred_element_type=F32,
        )
    down, copies = across_heads(down, down_share, down_in, tp_send.at[1], tp_recv.at[1], tp_count)
    flights.append(copies)
    result[...] = (mixed_in + down).astype(jnp.bfloat16)
    for flight in flights + [square_flight] + up_flights + down_flights:
        for copy in flight:
            copy.wait_send()


def vmem(count):
    return [pl.BlockSpec(memory_space=pltpu.VMEM)] * count


def local(
    kv,
    tp,
    tokens,
    mix_gain,
    query_weight,
    key_weight,
    value_weight,
    beta_weight,
    decay_weight,
    decay_rate,
    prior_state,
    tail_keys,
    tail_values,
    tail_beta,
    tail_decay,
    lengths,
    out_weight,
    mlp_gain,
    up_weight,
    down_weight,
):
    rows, heads, head_dim = prior_state.shape[:3]
    span = tail_keys.shape[2]
    batch = rows * kv
    depth = mix_gain.shape[0]
    width = depth * kv
    inner = heads * head_dim
    units = up_weight.shape[1]
    piece = min(units, 1024)
    pieces = units // piece
    dma = pltpu.SemaphoreType.DMA
    token_rows = lax.all_gather(tokens, "tp", axis=1, tiled=True)
    small_weight = jnp.concatenate(
        [beta_weight, decay_weight, jnp.zeros((depth, 128 - 2 * heads), jnp.bfloat16)], axis=1
    )
    query_s, key_s, value_s, small_s = pl.pallas_call(
        functools.partial(project_kernel, kv, heads),
        out_shape=[jax.ShapeDtypeStruct((rows, inner), F32)] * 3 + [jax.ShapeDtypeStruct((rows, 128), F32)],
        in_specs=vmem(6),
        out_specs=vmem(4),
        scratch_shapes=[
            pltpu.VMEM((kv, rows, 128), F32),
            pltpu.VMEM((kv, rows, 128), F32),
            pltpu.VMEM((3, kv, rows, inner), LINK),
            pltpu.VMEM((3, kv, rows, inner), LINK),
            dma((4, kv)),
            dma((4, kv)),
        ],
        compiler_params=pltpu.CompilerParams(
            collective_id=0, has_side_effects=True, vmem_limit_bytes=16 * 2**20
        ),
        name="project",
    )(token_rows, mix_gain.reshape(1, depth), query_weight, key_weight, value_weight, small_weight)
    count = rows * heads * span
    head_out = pl.pallas_call(
        functools.partial(delta_kernel, width),
        out_shape=jax.ShapeDtypeStruct((rows, inner), jnp.bfloat16),
        in_specs=vmem(4) + [pl.BlockSpec(memory_space=pltpu.SMEM)] + vmem(6),
        out_specs=vmem(1)[0],
        scratch_shapes=[
            pltpu.VMEM((count, head_dim), F32),
            pltpu.VMEM((count, head_dim), F32),
            pltpu.VMEM((rows * heads, head_dim), F32),
        ],
        compiler_params=pltpu.CompilerParams(vmem_limit_bytes=32 * 2**20),
        name="delta",
    )(
        query_s,
        key_s,
        value_s,
        small_s,
        decay_rate.reshape(1, heads),
        lengths.reshape(rows, 1),
        tail_beta,
        tail_decay,
        tail_keys.reshape(count, head_dim),
        tail_values.reshape(count, head_dim),
        prior_state,
    )
    slots = 2 + 2 * pieces
    result = pl.pallas_call(
        functools.partial(mixer_kernel, kv, tp, width),
        out_shape=jax.ShapeDtypeStruct((batch, depth), jnp.bfloat16),
        in_specs=vmem(6),
        out_specs=vmem(1)[0],
        scratch_shapes=[
            pltpu.VMEM((kv, rows, inner), jnp.bfloat16),
            pltpu.VMEM((batch, depth), F32),
            pltpu.VMEM((tp, batch, depth), F32),
            pltpu.VMEM((batch, depth), F32),
            pltpu.VMEM((tp, batch, depth), F32),
            pltpu.VMEM((kv, rows, 128), F32),
            pltpu.VMEM((kv, rows, 128), F32),
            pltpu.VMEM((pieces, kv, rows, piece), LINK),
            pltpu.VMEM((pieces, kv, rows, piece), LINK),
            pltpu.VMEM((pieces, rows, piece), jnp.bfloat16),
            pltpu.VMEM((pieces, kv, rows, piece), jnp.bfloat16),
            dma((slots, kv)),
            dma((slots, kv)),
            dma((2, tp)),
            dma((2, tp)),
        ],
        compiler_params=pltpu.CompilerParams(
            collective_id=1, has_side_effects=True, vmem_limit_bytes=32 * 2**20
        ),
        name="mixer",
    )(head_out, token_rows, mlp_gain.reshape(1, depth), out_weight, up_weight, down_weight)
    columns = depth // tp
    return lax.dynamic_slice_in_dim(result, lax.axis_index("tp") * columns, columns, axis=1)


def solution(mesh):
    in_specs = (
        P(None, ("kv", "tp")),
        P("kv"),
        P("kv", "tp"),
        P("kv", "tp"),
        P("kv", "tp"),
        P("kv", "tp"),
        P("kv", "tp"),
        P("tp"),
        P("kv", "tp", None, None),
        P("kv", "tp", None, None),
        P("kv", "tp", None, None),
        P("kv", "tp", None),
        P("kv", "tp", None),
        P("kv"),
        P("tp", "kv"),
        P("kv"),
        P("kv", "tp"),
        P("tp", "kv"),
    )
    out_specs = P(None, ("kv", "tp"))
    body = functools.partial(local, mesh.shape["kv"], mesh.shape["tp"])
    return jax.shard_map(body, mesh=mesh, in_specs=in_specs, out_specs=out_specs, check_vma=False)
```

```python
import functools
import math

import jax
import jax.numpy as jnp
from jax import lax
from jax.experimental import pallas as pl
from jax.experimental.pallas import tpu as pltpu
from jax.sharding import PartitionSpec as P

epsilon = 1e-06
LINK = jnp.bfloat16
F32 = jnp.float32
MESH = pl.DeviceIdType.MESH


def peer_of(axis, offset, count):
    return lax.rem(lax.axis_index(axis) + offset, count)


def greet(count, tp_count):
    barrier = pltpu.get_barrier_semaphore()
    group = group_of(count)
    met = [{"kv": inner_peer(offset, count)} for offset in range(1, group)]
    met += [{"kv": outer_peer(offset, count)} for offset in range(1, count // group)]
    met += [{"tp": peer_of("tp", offset, tp_count)} for offset in range(1, tp_count)]
    for peer in met:
        pl.semaphore_signal(barrier, inc=1, device_id=peer, device_id_type=MESH)
    return len(met)


def greeted(met):
    pl.semaphore_wait(pltpu.get_barrier_semaphore(), met)


def send(src, dst, send_sem, recv_sem, axis, peer):
    copy = pltpu.make_async_remote_copy(
        src_ref=src,
        dst_ref=dst,
        send_sem=send_sem,
        recv_sem=recv_sem,
        device_id={axis: peer},
        device_id_type=MESH,
    )
    copy.start()
    return copy


def group_of(count):
    return max(size for size in range(1, math.isqrt(count) + 1) if count % size == 0)


def place(count):
    group = group_of(count)
    me = lax.axis_index("kv")
    return me // group, lax.rem(me, group)


def inner_peer(offset, count):
    outer, inner = place(count)
    group = group_of(count)
    return outer * group + lax.rem(inner + offset, group)


def outer_peer(offset, count):
    outer, inner = place(count)
    group = group_of(count)
    return lax.rem(outer + offset, count // group) * group + inner


def put_rows(parts, block, count):
    group = group_of(count)
    rows = block.shape[0] // count
    split = block.reshape(count // group, group, rows, block.shape[1])
    for inner in range(group):
        parts[inner] = split[:, inner].astype(parts.dtype)


def scatter_inner(parts, arrivals, send_sems, recv_sems, count):
    group = group_of(count)
    _, inner = place(count)
    return [
        send(
            parts.at[lax.rem(inner + offset, group)],
            arrivals.at[offset],
            send_sems.at[offset],
            recv_sems.at[offset],
            "kv",
            inner_peer(offset, count),
        )
        for offset in range(1, group)
    ]


def scatter_outer(parts, arrivals, middle, middle_in, copies, send_sems, recv_sems, count):
    group = group_of(count)
    outer, inner = place(count)
    total = parts[inner].astype(F32)
    for offset in range(1, group):
        copies[offset - 1].wait_recv()
        total = total + arrivals[offset].astype(F32)
    middle[...] = total.astype(middle.dtype)
    return [
        send(
            middle.at[lax.rem(outer + offset, count // group)],
            middle_in.at[offset],
            send_sems.at[offset],
            recv_sems.at[offset],
            "kv",
            outer_peer(offset, count),
        )
        for offset in range(1, count // group)
    ]


def gathered_sum(middle, middle_in, copies, count):
    outer, _ = place(count)
    total = middle[outer].astype(F32)
    for offset, copy in enumerate(copies, 1):
        copy.wait_recv()
        total = total + middle_in[offset].astype(F32)
    return total


def gather_outer(everywhere, send_sems, recv_sems, count):
    outer, inner = place(count)
    block = everywhere.at[inner, outer]
    return [
        send(block, block, send_sems.at[offset], recv_sems.at[offset], "kv", outer_peer(offset, count))
        for offset in range(1, count // group_of(count))
    ]


def gather_inner(everywhere, copies, send_sems, recv_sems, count):
    _, inner = place(count)
    for copy in copies:
        copy.wait_recv()
    block = everywhere.at[inner]
    return [
        send(block, block, send_sems.at[offset], recv_sems.at[offset], "kv", inner_peer(offset, count))
        for offset in range(1, group_of(count))
    ]


def all_rows(everywhere):
    block = everywhere[...].astype(F32)
    group, outer, rows, width = block.shape
    return block.reshape(group * outer * rows, width).astype(jnp.bfloat16)


def in_order(block, count):
    group = group_of(count)
    outer = count // group
    split = block.reshape(group, outer, block.shape[0] // count, block.shape[1])
    return jnp.concatenate([split[i, o] for o in range(outer) for i in range(group)], axis=0)


def project_kernel(
    count,
    heads,
    tokens,
    gain,
    query_w,
    key_w,
    value_w,
    small_w,
    query_o,
    key_o,
    value_o,
    small_o,
    small_parts,
    small_in,
    small_mid,
    small_mid_in,
    parts,
    arrivals,
    middle,
    middle_in,
    send_sems,
    recv_sems,
):
    met = greet(count, 1)
    token_float = tokens[...].astype(F32)
    normed = (token_float * gain[...]).astype(jnp.bfloat16)
    small = jnp.dot(normed, small_w[...], preferred_element_type=F32)
    squares = jnp.sum(token_float * token_float, axis=1, keepdims=True)
    lane = lax.broadcasted_iota(jnp.int32, small.shape, 1)
    put_rows(small_parts, jnp.where(lane == 2 * heads, squares, small), count)
    greeted(met)
    bufs = [(small_parts, small_in, small_mid, small_mid_in)]
    bufs += [tuple(ref.at[p] for ref in (parts, arrivals, middle, middle_in)) for p in range(3)]
    first = [scatter_inner(*bufs[0][:2], send_sems.at[0], recv_sems.at[0], count)]
    for p, weight in enumerate((query_w, key_w, value_w), 1):
        put_rows(bufs[p][0], jnp.dot(normed, weight[...], preferred_element_type=F32), count)
        first.append(scatter_inner(*bufs[p][:2], send_sems.at[p], recv_sems.at[p], count))
    second = [
        scatter_outer(*bufs[p], first[p], send_sems.at[4 + p], recv_sems.at[4 + p], count) for p in range(4)
    ]
    for p, out in enumerate((small_o, query_o, key_o, value_o)):
        out[...] = gathered_sum(bufs[p][2], bufs[p][3], second[p], count)
    for flight in first + second:
        for copy in flight:
            copy.wait_send()


def unit_rows(vectors):
    return vectors * lax.rsqrt(jnp.sum(vectors * vectors, axis=-1, keepdims=True) + epsilon)


def silu(x):
    return x * jax.nn.sigmoid(x)


def softplus(x):
    return jnp.maximum(x, 0.0) + jnp.log(1.0 + jnp.exp(-jnp.abs(x)))


def delta_kernel(
    width,
    query_r,
    key_r,
    value_r,
    small_r,
    rate,
    lengths,
    betas,
    decays,
    keys,
    values,
    state,
    out,
    keys32,
    values32,
    rows_scr,
    held,
    held_sem,
):
    fetch = pltpu.make_async_copy(state, held, held_sem)
    fetch.start()
    rows, heads, head_dim = state.shape[0], state.shape[1], state.shape[2]
    span = betas.shape[2]

    def stack(pieces):
        return jnp.concatenate(pieces, axis=0)

    keys32[...] = keys[...].astype(F32)
    values32[...] = values[...].astype(F32)
    small = small_r[...]
    scale = lax.rsqrt(small[:, 2 * heads : 2 * heads + 1] / width + epsilon)
    scaled = small * scale

    def by_heads(ref):
        raw = ref[...] * scale
        return stack([raw[:, h * head_dim : (h + 1) * head_dim] for h in range(heads)])

    queries = unit_rows(silu(by_heads(query_r)))
    new_key = unit_rows(silu(by_heads(key_r)))
    new_value = silu(by_heads(value_r))
    new_beta = stack([jax.nn.sigmoid(scaled[:, h : h + 1]) for h in range(heads)])
    new_decay = stack(
        [-rate[0, h] * softplus(scaled[:, heads + h : heads + h + 1]) for h in range(heads)]
    )
    live = lax.broadcasted_iota(jnp.int32, (rows, span), 1) < lengths[...]
    beta_live = stack([jnp.where(live, betas[:, h, :], 0.0) for h in range(heads)])
    shrink = stack([jnp.exp(jnp.where(live, decays[:, h, :], 0.0)) for h in range(heads)])

    meet = new_beta * jnp.sum(new_key * queries, axis=1, keepdims=True)
    fade = jnp.exp(new_decay)
    probe = (queries - meet * new_key) * fade
    read = meet * new_value
    for t in range(span - 1, -1, -1):
        k = stack([keys32[pl.ds(h * span + t, rows, stride=heads * span), :] for h in range(heads)])
        v = stack([values32[pl.ds(h * span + t, rows, stride=heads * span), :] for h in range(heads)])
        inverse = lax.rsqrt(jnp.sum(k * k, axis=1, keepdims=True) + epsilon)
        unit = k * inverse
        hit = beta_live[:, t : t + 1] * jnp.sum(unit * probe, axis=1, keepdims=True)
        read = read + hit * v
        probe = shrink[:, t : t + 1] * (probe - hit * unit)
    total = rows * heads
    if total < head_dim:
        probe = jnp.concatenate([probe, jnp.zeros((head_dim - total, head_dim), F32)], axis=0)
    columns = probe.T
    fetch.wait()
    for h in range(heads):
        for r in range(rows):
            n = h * rows + r
            rows_scr[n : n + 1, :] = jnp.sum(columns[:, n : n + 1] * held[r, h], axis=0, keepdims=True)
    final = read + rows_scr[...]
    for h in range(heads):
        out[:, h * head_dim : (h + 1) * head_dim] = final[h * rows : (h + 1) * rows].astype(jnp.bfloat16)


def across_heads(block, mine, arrivals, send_sems, recv_sems, count):
    mine[...] = block
    copies = []
    for offset in range(1, count):
        peer = peer_of("tp", offset, count)
        copies.append(send(mine, arrivals.at[offset], send_sems.at[offset], recv_sems.at[offset], "tp", peer))
    total = block
    for offset in range(1, count):
        copies[offset - 1].wait_recv()
        total = total + arrivals[offset]
    return total, copies


def mixer_kernel(
    count,
    tp_count,
    width,
    head_out,
    tokens,
    gain,
    out_w,
    up_w,
    down_w,
    result,
    heads_all,
    share,
    share_in,
    down_share,
    down_in,
    square_parts,
    square_in,
    square_mid,
    square_mid_in,
    parts,
    arrivals,
    middle,
    middle_in,
    hidden_all,
    kv_send,
    kv_recv,
    tp_send,
    tp_recv,
):
    pieces, piece = parts.shape[0], parts.shape[4]
    outer, inner = place(count)
    slots = iter(range(kv_send.shape[0]))

    def sems():
        slot = next(slots)
        return kv_send.at[slot], kv_recv.at[slot]

    met = greet(count, tp_count)
    heads_all[inner, outer] = head_out[...]
    greeted(met)
    flights = [gather_outer(heads_all, *sems(), count)]
    flights.append(gather_inner(heads_all, flights[0], *sems(), count))
    for copy in flights[1]:
        copy.wait_recv()
    attended = jnp.dot(all_rows(heads_all), out_w[...], preferred_element_type=F32)
    attended, copies = across_heads(
        in_order(attended, count), share, share_in, tp_send.at[0], tp_recv.at[0], tp_count
    )
    flights.append(copies)
    mixed_in = (tokens[...].astype(F32) + attended).astype(jnp.bfloat16).astype(F32)
    squares = jnp.sum(mixed_in * mixed_in, axis=1, keepdims=True)
    bufs = [tuple(ref.at[p] for ref in (parts, arrivals, middle, middle_in)) for p in range(pieces)]
    bufs.append((square_parts, square_in, square_mid, square_mid_in))
    put_rows(square_parts, jnp.broadcast_to(squares, (squares.shape[0], 128)), count)
    square_first = scatter_inner(square_parts, square_in, *sems(), count)
    normed = (mixed_in * gain[...]).astype(jnp.bfloat16)
    first = []
    for p in range(pieces):
        block = jnp.dot(normed, up_w[:, p * piece : (p + 1) * piece], preferred_element_type=F32)
        put_rows(bufs[p][0], block, count)
        first.append(scatter_inner(*bufs[p][:2], *sems(), count))
    square_second = scatter_outer(*bufs[pieces], square_first, *sems(), count)
    second = [scatter_outer(*bufs[p], first[p], *sems(), count) for p in range(pieces)]
    own_squares = gathered_sum(square_mid, square_mid_in, square_second, count)
    scale = lax.rsqrt(own_squares[:, :1] / width + epsilon)
    third = []
    for p in range(pieces):
        raw = gathered_sum(bufs[p][2], bufs[p][3], second[p], count) * scale
        hidden_all[p, inner, outer] = jnp.square(jnp.maximum(raw, 0.0)).astype(jnp.bfloat16)
        third.append(gather_outer(hidden_all.at[p], *sems(), count))
    fourth = [gather_inner(hidden_all.at[p], third[p], *sems(), count) for p in range(pieces)]
    down = jnp.zeros(share.shape, F32)
    for p in range(pieces):
        for copy in fourth[p]:
            copy.wait_recv()
        down = down + jnp.dot(
            all_rows(hidden_all.at[p]),
            down_w[p * piece : (p + 1) * piece, :],
            preferred_element_type=F32,
        )
    down, copies = across_heads(
        in_order(down, count), down_share, down_in, tp_send.at[1], tp_recv.at[1], tp_count
    )
    flights.append(copies)
    result[...] = (mixed_in + down).astype(jnp.bfloat16)
    for flight in flights + [square_first, square_second] + first + second + third + fourth:
        for copy in flight:
            copy.wait_send()


def vmem(count):
    return [pl.BlockSpec(memory_space=pltpu.VMEM)] * count


def local(
    kv,
    tp,
    tokens,
    mix_gain,
    query_weight,
    key_weight,
    value_weight,
    beta_weight,
    decay_weight,
    decay_rate,
    prior_state,
    tail_keys,
    tail_values,
    tail_beta,
    tail_decay,
    lengths,
    out_weight,
    mlp_gain,
    up_weight,
    down_weight,
):
    rows, heads, head_dim = prior_state.shape[:3]
    span = tail_keys.shape[2]
    batch = rows * kv
    depth = mix_gain.shape[0]
    width = depth * kv
    inner = heads * head_dim
    units = up_weight.shape[1]
    piece = min(units, 1024)
    pieces = units // piece
    dma = pltpu.SemaphoreType.DMA
    group = group_of(kv)

    def scatter_buffers(lead, columns, dtype):
        full = pltpu.VMEM(lead + (group, kv // group, rows, columns), dtype)
        middle = pltpu.VMEM(lead + (kv // group, rows, columns), dtype)
        return full, full, middle, middle

    token_rows = lax.all_gather(tokens, "tp", axis=1, tiled=True)
    small_weight = jnp.concatenate(
        [beta_weight, decay_weight, jnp.zeros((depth, 128 - 2 * heads), jnp.bfloat16)], axis=1
    )
    query_s, key_s, value_s, small_s = pl.pallas_call(
        functools.partial(project_kernel, kv, heads),
        out_shape=[jax.ShapeDtypeStruct((rows, inner), F32)] * 3 + [jax.ShapeDtypeStruct((rows, 128), F32)],
        in_specs=vmem(6),
        out_specs=vmem(4),
        scratch_shapes=[
            *scatter_buffers((), 128, F32),
            *scatter_buffers((3,), inner, LINK),
            dma((8, kv)),
            dma((8, kv)),
        ],
        compiler_params=pltpu.CompilerParams(
            collective_id=0, has_side_effects=True, vmem_limit_bytes=12 * 2**20
        ),
        cost_estimate=pl.CostEstimate(flops=2 * 10**10, bytes_accessed=0, transcendentals=0),
        name="project",
    )(token_rows, mix_gain.reshape(1, depth), query_weight, key_weight, value_weight, small_weight)
    count = rows * heads * span
    head_out = pl.pallas_call(
        functools.partial(delta_kernel, width),
        out_shape=jax.ShapeDtypeStruct((rows, inner), jnp.bfloat16),
        in_specs=vmem(4) + [pl.BlockSpec(memory_space=pltpu.SMEM)]
        + vmem(5)
        + [pl.BlockSpec(memory_space=pl.ANY)],
        out_specs=vmem(1)[0],
        scratch_shapes=[
            pltpu.VMEM((count, head_dim), F32),
            pltpu.VMEM((count, head_dim), F32),
            pltpu.VMEM((rows * heads, head_dim), F32),
            pltpu.VMEM(prior_state.shape, F32),
            pltpu.SemaphoreType.DMA,
        ],
        compiler_params=pltpu.CompilerParams(vmem_limit_bytes=57 * 2**20),
        name="delta",
    )(
        query_s,
        key_s,
        value_s,
        small_s,
        decay_rate.reshape(1, heads),
        lengths.reshape(rows, 1),
        tail_beta,
        tail_decay,
        tail_keys.reshape(count, head_dim),
        tail_values.reshape(count, head_dim),
        prior_state,
    )
    slots = 4 + 4 * pieces
    result = pl.pallas_call(
        functools.partial(mixer_kernel, kv, tp, width),
        out_shape=jax.ShapeDtypeStruct((batch, depth), jnp.bfloat16),
        in_specs=vmem(6),
        out_specs=vmem(1)[0],
        scratch_shapes=[
            pltpu.VMEM((group, kv // group, rows, inner), jnp.bfloat16),
            pltpu.VMEM((batch, depth), F32),
            pltpu.VMEM((tp, batch, depth), F32),
            pltpu.VMEM((batch, depth), F32),
            pltpu.VMEM((tp, batch, depth), F32),
            *scatter_buffers((), 128, F32),
            *scatter_buffers((pieces,), piece, LINK),
            pltpu.VMEM((pieces, group, kv // group, rows, piece), jnp.bfloat16),
            dma((slots, kv)),
            dma((slots, kv)),
            dma((2, tp)),
            dma((2, tp)),
        ],
        compiler_params=pltpu.CompilerParams(
            collective_id=1, has_side_effects=True, vmem_limit_bytes=20 * 2**20
        ),
        name="mixer",
    )(head_out, token_rows, mlp_gain.reshape(1, depth), out_weight, up_weight, down_weight)
    columns = depth // tp
    return lax.dynamic_slice_in_dim(result, lax.axis_index("tp") * columns, columns, axis=1)


def solution(mesh):
    in_specs = (
        P(None, ("kv", "tp")),
        P("kv"),
        P("kv", "tp"),
        P("kv", "tp"),
        P("kv", "tp"),
        P("kv", "tp"),
        P("kv", "tp"),
        P("tp"),
        P("kv", "tp", None, None),
        P("kv", "tp", None, None),
        P("kv", "tp", None, None),
        P("kv", "tp", None),
        P("kv", "tp", None),
        P("kv"),
        P("tp", "kv"),
        P("kv"),
        P("kv", "tp"),
        P("tp", "kv"),
    )
    out_specs = P(None, ("kv", "tp"))
    body = functools.partial(local, mesh.shape["kv"], mesh.shape["tp"])
    return jax.shard_map(body, mesh=mesh, in_specs=in_specs, out_specs=out_specs, check_vma=False)
```

```python
import functools
import math

import jax
import jax.numpy as jnp
from jax import lax
from jax.experimental import pallas as pl
from jax.experimental.pallas import tpu as pltpu
from jax.sharding import PartitionSpec as P

epsilon = 1e-06
LINK = jnp.bfloat16
F32 = jnp.float32
MESH = pl.DeviceIdType.MESH


def peer_of(axis, offset, count):
    return lax.rem(lax.axis_index(axis) + offset, count)


def greet(count, tp_count):
    barrier = pltpu.get_barrier_semaphore()
    group = group_of(count)
    met = [{"kv": inner_peer(offset, count)} for offset in range(1, group)]
    met += [{"kv": outer_peer(offset, count)} for offset in range(1, count // group)]
    met += [{"tp": peer_of("tp", offset, tp_count)} for offset in range(1, tp_count)]
    for peer in met:
        pl.semaphore_signal(barrier, inc=1, device_id=peer, device_id_type=MESH)
    return len(met)


def greeted(met):
    pl.semaphore_wait(pltpu.get_barrier_semaphore(), met)


def send(src, dst, send_sem, recv_sem, axis, peer):
    copy = pltpu.make_async_remote_copy(
        src_ref=src,
        dst_ref=dst,
        send_sem=send_sem,
        recv_sem=recv_sem,
        device_id={axis: peer},
        device_id_type=MESH,
    )
    copy.start()
    return copy


def group_of(count):
    return max(size for size in range(1, math.isqrt(count) + 1) if count % size == 0)


def place(count):
    group = group_of(count)
    me = lax.axis_index("kv")
    return me // group, lax.rem(me, group)


def inner_peer(offset, count):
    outer, inner = place(count)
    group = group_of(count)
    return outer * group + lax.rem(inner + offset, group)


def outer_peer(offset, count):
    outer, inner = place(count)
    group = group_of(count)
    return lax.rem(outer + offset, count // group) * group + inner


def put_rows(parts, block, count):
    group = group_of(count)
    rows = block.shape[0] // count
    split = block.reshape(count // group, group, rows, block.shape[1])
    for inner in range(group):
        parts[inner] = split[:, inner].astype(parts.dtype)


def scatter_inner(parts, arrivals, send_sems, recv_sems, count):
    group = group_of(count)
    _, inner = place(count)
    return [
        send(
            parts.at[lax.rem(inner + offset, group)],
            arrivals.at[offset],
            send_sems.at[offset],
            recv_sems.at[offset],
            "kv",
            inner_peer(offset, count),
        )
        for offset in range(1, group)
    ]


def scatter_outer(parts, arrivals, middle, middle_in, copies, send_sems, recv_sems, count):
    group = group_of(count)
    outer, inner = place(count)
    total = parts[inner].astype(F32)
    for offset in range(1, group):
        copies[offset - 1].wait_recv()
        total = total + arrivals[offset].astype(F32)
    middle[...] = total.astype(middle.dtype)
    return [
        send(
            middle.at[lax.rem(outer + offset, count // group)],
            middle_in.at[offset],
            send_sems.at[offset],
            recv_sems.at[offset],
            "kv",
            outer_peer(offset, count),
        )
        for offset in range(1, count // group)
    ]


def gathered_sum(middle, middle_in, copies, count):
    outer, _ = place(count)
    total = middle[outer].astype(F32)
    for offset, copy in enumerate(copies, 1):
        copy.wait_recv()
        total = total + middle_in[offset].astype(F32)
    return total


def gather_outer(everywhere, send_sems, recv_sems, count):
    outer, inner = place(count)
    block = everywhere.at[inner, outer]
    return [
        send(block, block, send_sems.at[offset], recv_sems.at[offset], "kv", outer_peer(offset, count))
        for offset in range(1, count // group_of(count))
    ]


def gather_inner(everywhere, copies, send_sems, recv_sems, count):
    _, inner = place(count)
    for copy in copies:
        copy.wait_recv()
    block = everywhere.at[inner]
    return [
        send(block, block, send_sems.at[offset], recv_sems.at[offset], "kv", inner_peer(offset, count))
        for offset in range(1, group_of(count))
    ]


def all_rows(everywhere):
    block = everywhere[...].astype(F32)
    group, outer, rows, width = block.shape
    return block.reshape(group * outer * rows, width).astype(jnp.bfloat16)


def in_order(block, count):
    group = group_of(count)
    outer = count // group
    split = block.reshape(group, outer, block.shape[0] // count, block.shape[1])
    return jnp.concatenate([split[i, o] for o in range(outer) for i in range(group)], axis=0)


def project_kernel(
    count,
    heads,
    tokens,
    gain,
    query_w,
    key_w,
    value_w,
    small_w,
    query_o,
    key_o,
    value_o,
    small_o,
    small_parts,
    small_in,
    small_mid,
    small_mid_in,
    parts,
    arrivals,
    middle,
    middle_in,
    send_sems,
    recv_sems,
):
    met = greet(count, 1)
    token_float = tokens[...].astype(F32)
    normed = (token_float * gain[...]).astype(jnp.bfloat16)
    small = jnp.dot(normed, small_w[...], preferred_element_type=F32)
    squares = jnp.sum(token_float * token_float, axis=1, keepdims=True)
    lane = lax.broadcasted_iota(jnp.int32, small.shape, 1)
    put_rows(small_parts, jnp.where(lane == 2 * heads, squares, small), count)
    greeted(met)
    bufs = [(small_parts, small_in, small_mid, small_mid_in)]
    bufs += [tuple(ref.at[p] for ref in (parts, arrivals, middle, middle_in)) for p in range(3)]
    first = [scatter_inner(*bufs[0][:2], send_sems.at[0], recv_sems.at[0], count)]
    for p, weight in enumerate((query_w, key_w, value_w), 1):
        put_rows(bufs[p][0], jnp.dot(normed, weight[...], preferred_element_type=F32), count)
        first.append(scatter_inner(*bufs[p][:2], send_sems.at[p], recv_sems.at[p], count))
    second = [
        scatter_outer(*bufs[p], first[p], send_sems.at[4 + p], recv_sems.at[4 + p], count) for p in range(4)
    ]
    for p, out in enumerate((small_o, query_o, key_o, value_o)):
        out[...] = gathered_sum(bufs[p][2], bufs[p][3], second[p], count)
    for flight in first + second:
        for copy in flight:
            copy.wait_send()


def unit_rows(vectors):
    return vectors * lax.rsqrt(jnp.sum(vectors * vectors, axis=-1, keepdims=True) + epsilon)


def silu(x):
    return x * jax.nn.sigmoid(x)


def softplus(x):
    return jnp.maximum(x, 0.0) + jnp.log(1.0 + jnp.exp(-jnp.abs(x)))


def delta_kernel(
    width,
    query_r,
    key_r,
    value_r,
    small_r,
    rate,
    lengths,
    betas,
    decays,
    keys,
    values,
    state,
    out,
    keys32,
    values32,
    rows_scr,
    held,
    held_sem,
):
    fetch = pltpu.make_async_copy(state, held, held_sem)
    fetch.start()
    rows, heads, head_dim = state.shape[0], state.shape[1], state.shape[2]
    span = betas.shape[2]

    def stack(pieces):
        return jnp.concatenate(pieces, axis=0)

    keys32[...] = keys[...].astype(F32)
    values32[...] = values[...].astype(F32)
    small = small_r[...]
    scale = lax.rsqrt(small[:, 2 * heads : 2 * heads + 1] / width + epsilon)
    scaled = small * scale

    def by_heads(ref):
        raw = ref[...] * scale
        return stack([raw[:, h * head_dim : (h + 1) * head_dim] for h in range(heads)])

    queries = unit_rows(silu(by_heads(query_r)))
    new_key = unit_rows(silu(by_heads(key_r)))
    new_value = silu(by_heads(value_r))
    new_beta = stack([jax.nn.sigmoid(scaled[:, h : h + 1]) for h in range(heads)])
    new_decay = stack(
        [-rate[0, h] * softplus(scaled[:, heads + h : heads + h + 1]) for h in range(heads)]
    )
    live = lax.broadcasted_iota(jnp.int32, (rows, span), 1) < lengths[...]
    beta_live = stack([jnp.where(live, betas[:, h, :], 0.0) for h in range(heads)])
    shrink = stack([jnp.exp(jnp.where(live, decays[:, h, :], 0.0)) for h in range(heads)])

    meet = new_beta * jnp.sum(new_key * queries, axis=1, keepdims=True)
    fade = jnp.exp(new_decay)
    probe = (queries - meet * new_key) * fade
    read = meet * new_value
    for t in range(span - 1, -1, -1):
        k = stack([keys32[pl.ds(h * span + t, rows, stride=heads * span), :] for h in range(heads)])
        v = stack([values32[pl.ds(h * span + t, rows, stride=heads * span), :] for h in range(heads)])
        inverse = lax.rsqrt(jnp.sum(k * k, axis=1, keepdims=True) + epsilon)
        unit = k * inverse
        hit = beta_live[:, t : t + 1] * jnp.sum(unit * probe, axis=1, keepdims=True)
        read = read + hit * v
        probe = shrink[:, t : t + 1] * (probe - hit * unit)
    total = rows * heads
    if total < head_dim:
        probe = jnp.concatenate([probe, jnp.zeros((head_dim - total, head_dim), F32)], axis=0)
    columns = probe.T
    fetch.wait()
    for h in range(heads):
        for r in range(rows):
            n = h * rows + r
            rows_scr[n : n + 1, :] = jnp.sum(columns[:, n : n + 1] * held[r, h], axis=0, keepdims=True)
    final = read + rows_scr[...]
    for h in range(heads):
        out[:, h * head_dim : (h + 1) * head_dim] = final[h * rows : (h + 1) * rows].astype(jnp.bfloat16)


def across_heads(block, mine, arrivals, send_sems, recv_sems, count):
    mine[...] = block
    copies = []
    for offset in range(1, count):
        peer = peer_of("tp", offset, count)
        copies.append(send(mine, arrivals.at[offset], send_sems.at[offset], recv_sems.at[offset], "tp", peer))
    total = block
    for offset in range(1, count):
        copies[offset - 1].wait_recv()
        total = total + arrivals[offset]
    return total, copies


def mixer_kernel(
    count,
    tp_count,
    width,
    head_out,
    tokens,
    gain,
    out_w,
    up_w,
    down_w,
    result,
    heads_all,
    share,
    share_in,
    down_share,
    down_in,
    square_parts,
    square_in,
    square_mid,
    square_mid_in,
    parts,
    arrivals,
    middle,
    middle_in,
    hidden_all,
    kv_send,
    kv_recv,
    tp_send,
    tp_recv,
):
    pieces, piece = parts.shape[0], parts.shape[4]
    outer, inner = place(count)
    slots = iter(range(kv_send.shape[0]))

    def sems():
        slot = next(slots)
        return kv_send.at[slot], kv_recv.at[slot]

    met = greet(count, tp_count)
    heads_all[inner, outer] = head_out[...]
    greeted(met)
    flights = [gather_outer(heads_all, *sems(), count)]
    flights.append(gather_inner(heads_all, flights[0], *sems(), count))
    for copy in flights[1]:
        copy.wait_recv()
    attended = jnp.dot(all_rows(heads_all), out_w[...], preferred_element_type=F32)
    attended, copies = across_heads(
        in_order(attended, count), share, share_in, tp_send.at[0], tp_recv.at[0], tp_count
    )
    flights.append(copies)
    mixed_in = (tokens[...].astype(F32) + attended).astype(jnp.bfloat16).astype(F32)
    squares = jnp.sum(mixed_in * mixed_in, axis=1, keepdims=True)
    bufs = [tuple(ref.at[p] for ref in (parts, arrivals, middle, middle_in)) for p in range(pieces)]
    bufs.append((square_parts, square_in, square_mid, square_mid_in))
    put_rows(square_parts, jnp.broadcast_to(squares, (squares.shape[0], 128)), count)
    square_first = scatter_inner(square_parts, square_in, *sems(), count)
    normed = (mixed_in * gain[...]).astype(jnp.bfloat16)
    first = []
    for p in range(pieces):
        block = jnp.dot(normed, up_w[:, p * piece : (p + 1) * piece], preferred_element_type=F32)
        put_rows(bufs[p][0], block, count)
        first.append(scatter_inner(*bufs[p][:2], *sems(), count))
    square_second = scatter_outer(*bufs[pieces], square_first, *sems(), count)
    second = [scatter_outer(*bufs[p], first[p], *sems(), count) for p in range(pieces)]
    own_squares = gathered_sum(square_mid, square_mid_in, square_second, count)
    scale = lax.rsqrt(own_squares[:, :1] / width + epsilon)
    third = []
    for p in range(pieces):
        raw = gathered_sum(bufs[p][2], bufs[p][3], second[p], count) * scale
        hidden_all[p, inner, outer] = jnp.square(jnp.maximum(raw, 0.0)).astype(jnp.bfloat16)
        third.append(gather_outer(hidden_all.at[p], *sems(), count))
    fourth = [gather_inner(hidden_all.at[p], third[p], *sems(), count) for p in range(pieces)]
    down = jnp.zeros(share.shape, F32)
    for p in range(pieces):
        for copy in fourth[p]:
            copy.wait_recv()
        down = down + jnp.dot(
            all_rows(hidden_all.at[p]),
            down_w[p * piece : (p + 1) * piece, :],
            preferred_element_type=F32,
        )
    down, copies = across_heads(
        in_order(down, count), down_share, down_in, tp_send.at[1], tp_recv.at[1], tp_count
    )
    flights.append(copies)
    result[...] = (mixed_in + down).astype(jnp.bfloat16)
    for flight in flights + [square_first, square_second] + first + second + third + fourth:
        for copy in flight:
            copy.wait_send()


def vmem(count):
    return [pl.BlockSpec(memory_space=pltpu.VMEM)] * count


def local(
    kv,
    tp,
    tokens,
    mix_gain,
    query_weight,
    key_weight,
    value_weight,
    beta_weight,
    decay_weight,
    decay_rate,
    prior_state,
    tail_keys,
    tail_values,
    tail_beta,
    tail_decay,
    lengths,
    out_weight,
    mlp_gain,
    up_weight,
    down_weight,
):
    rows, heads, head_dim = prior_state.shape[:3]
    span = tail_keys.shape[2]
    batch = rows * kv
    depth = mix_gain.shape[0]
    width = depth * kv
    inner = heads * head_dim
    units = up_weight.shape[1]
    piece = min(units, 1024)
    pieces = units // piece
    dma = pltpu.SemaphoreType.DMA
    group = group_of(kv)

    def scatter_buffers(lead, columns, dtype):
        full = pltpu.VMEM(lead + (group, kv // group, rows, columns), dtype)
        middle = pltpu.VMEM(lead + (kv // group, rows, columns), dtype)
        return full, full, middle, middle

    token_rows = lax.all_gather(tokens, "tp", axis=1, tiled=True)
    small_weight = jnp.concatenate(
        [beta_weight, decay_weight, jnp.zeros((depth, 128 - 2 * heads), jnp.bfloat16)], axis=1
    )
    query_s, key_s, value_s, small_s = pl.pallas_call(
        functools.partial(project_kernel, kv, heads),
        out_shape=[jax.ShapeDtypeStruct((rows, inner), F32)] * 3 + [jax.ShapeDtypeStruct((rows, 128), F32)],
        in_specs=vmem(6),
        out_specs=vmem(4),
        scratch_shapes=[
            *scatter_buffers((), 128, F32),
            *scatter_buffers((3,), inner, LINK),
            dma((8, kv)),
            dma((8, kv)),
        ],
        compiler_params=pltpu.CompilerParams(
            collective_id=0, has_side_effects=True, vmem_limit_bytes=57 * 2**20
        ),
        cost_estimate=pl.CostEstimate(flops=2 * 10**10, bytes_accessed=0, transcendentals=0),
        name="project",
    )(token_rows, mix_gain.reshape(1, depth), query_weight, key_weight, value_weight, small_weight)
    count = rows * heads * span
    head_out = pl.pallas_call(
        functools.partial(delta_kernel, width),
        out_shape=jax.ShapeDtypeStruct((rows, inner), jnp.bfloat16),
        in_specs=vmem(4) + [pl.BlockSpec(memory_space=pltpu.SMEM)]
        + vmem(5)
        + [pl.BlockSpec(memory_space=pl.ANY)],
        out_specs=vmem(1)[0],
        scratch_shapes=[
            pltpu.VMEM((count, head_dim), F32),
            pltpu.VMEM((count, head_dim), F32),
            pltpu.VMEM((rows * heads, head_dim), F32),
            pltpu.VMEM(prior_state.shape, F32),
            pltpu.SemaphoreType.DMA,
        ],
        compiler_params=pltpu.CompilerParams(vmem_limit_bytes=57 * 2**20),
        name="delta",
    )(
        query_s,
        key_s,
        value_s,
        small_s,
        decay_rate.reshape(1, heads),
        lengths.reshape(rows, 1),
        tail_beta,
        tail_decay,
        tail_keys.reshape(count, head_dim),
        tail_values.reshape(count, head_dim),
        prior_state,
    )
    slots = 4 + 4 * pieces
    result = pl.pallas_call(
        functools.partial(mixer_kernel, kv, tp, width),
        out_shape=jax.ShapeDtypeStruct((batch, depth), jnp.bfloat16),
        in_specs=vmem(6),
        out_specs=vmem(1)[0],
        scratch_shapes=[
            pltpu.VMEM((group, kv // group, rows, inner), jnp.bfloat16),
            pltpu.VMEM((batch, depth), F32),
            pltpu.VMEM((tp, batch, depth), F32),
            pltpu.VMEM((batch, depth), F32),
            pltpu.VMEM((tp, batch, depth), F32),
            *scatter_buffers((), 128, F32),
            *scatter_buffers((pieces,), piece, LINK),
            pltpu.VMEM((pieces, group, kv // group, rows, piece), jnp.bfloat16),
            dma((slots, kv)),
            dma((slots, kv)),
            dma((2, tp)),
            dma((2, tp)),
        ],
        compiler_params=pltpu.CompilerParams(
            collective_id=1, has_side_effects=True, vmem_limit_bytes=20 * 2**20
        ),
        name="mixer",
    )(head_out, token_rows, mlp_gain.reshape(1, depth), out_weight, up_weight, down_weight)
    columns = depth // tp
    return lax.dynamic_slice_in_dim(result, lax.axis_index("tp") * columns, columns, axis=1)


def solution(mesh):
    in_specs = (
        P(None, ("kv", "tp")),
        P("kv"),
        P("kv", "tp"),
        P("kv", "tp"),
        P("kv", "tp"),
        P("kv", "tp"),
        P("kv", "tp"),
        P("tp"),
        P("kv", "tp", None, None),
        P("kv", "tp", None, None),
        P("kv", "tp", None, None),
        P("kv", "tp", None),
        P("kv", "tp", None),
        P("kv"),
        P("tp", "kv"),
        P("kv"),
        P("kv", "tp"),
        P("tp", "kv"),
    )
    out_specs = P(None, ("kv", "tp"))
    body = functools.partial(local, mesh.shape["kv"], mesh.shape["tp"])
    return jax.shard_map(body, mesh=mesh, in_specs=in_specs, out_specs=out_specs, check_vma=False)
```
